32 devices in a mesh: ep: 16 (over z, y, core), tp: 2 (over x).
Axes of the slice: x: 2, y: 2, z: 4, core: 2. Of those that a mesh axis runs over, the one named last changes fastest.
Arguments:
- tokens: bfloat16 [256, 2048], P('ep'), may hold values from -6 to 6
- positions: int32 [256], P('ep'), may hold values from 1024 to 16383
- state: float32 [256, 4, 128, 128], P('ep', 'tp'), may hold values from -1 to 1
- mix_gain: float32 [2048], replicated, may hold values from 0.1 to 1.9
- w_query: bfloat16 [2048, 512], P(None, 'tp'), may hold values from -0.125 to 0.125
- w_key: bfloat16 [2048, 512], P(None, 'tp'), may hold values from -0.125 to 0.125
- w_value: bfloat16 [2048, 512], P(None, 'tp'), may hold values from -0.125 to 0.125
- w_out: bfloat16 [512, 2048], P('tp'), may hold values from -0.25 to 0.25
- ffn_gain: float32 [2048], replicated, may hold values from 0.1 to 1.9
- branch_gate: bfloat16 [2048], replicated, may hold values from -0.125 to 0.125
- dense_gate: bfloat16 [2048, 4096], P('tp', 'ep'), may hold values from -0.125 to 0.125
- dense_up: bfloat16 [2048, 4096], P('tp', 'ep'), may hold values from -0.125 to 0.125
- dense_down: bfloat16 [4096, 2048], P('ep', 'tp'), may hold values from -0.09375 to 0.09375
- routes: int32 [256, 6], P('ep'), may hold values from 0 to 15, all different within a row; in each aligned block of 16 rows (0 to 15, 16 to 31, ...) at most 12 rows name the same one
- route_scores: float32 [256, 6], P('ep'), may hold values from 0.05 to 1
- expert_gate: bfloat16 [16, 2048, 512], P('ep', None, 'tp'), may hold values from -0.125 to 0.125
- expert_up: bfloat16 [16, 2048, 512], P('ep', None, 'tp'), may hold values from -0.125 to 0.125
- expert_down: bfloat16 [16, 512, 2048], P('ep', 'tp'), may hold values from -0.25 to 0.25
Outputs:
- layer_out: bfloat16 [256, 2048], P('ep', 'tp')
The draws below stay inside these ranges and needn't reach their ends.
Inputs may be any that keep to these rules, and one draw needn't show every extreme that they name: `routes`: each row names 6 different experts. In each aligned block of 16 rows (the rows of one index of ep) no expert is named by more than 12 rows, a bound that some block reaches.
All inputs are finite; a program needn't handle non-finite values.
Results may differ from the reference program's by a relative error of at most 0.012.
Values may be sent and summed in bfloat16 or wider, within the bound.
A program may use at most 64 MiB of HBM per device.

```python
import math
import jax
import jax.numpy as jnp
import numpy as np
from jax import lax

D = 2048
HEADS = 4
HEAD = 128
EXPERT_W = 512
DENSE = 4096
TOP = 6
SEQ_DEV = 16
BATCH = 256
EXPERTS = 16
CAP = 12
N_EP = 16
N_TP = 2


def set_ends(result, stream_key, smallest, high):
    shape = result.shape
    spot = [jax.random.randint(jax.random.fold_in(stream_key, axis), (), 0, shape[axis]) for axis in range(len(shape))]
    result = result.at[tuple(spot)].set(smallest)
    longest = shape.index(max(shape))
    spot[longest] = (spot[longest] + 1) % shape[longest]
    return result.at[tuple(spot)].set(high)


def level_of(own_key, shape, split, smallest, top_value):
    gain, own = 1.0, jax.random.fold_in(own_key, 6)
    for axis_at, blocks in split:
        heights = jnp.exp(jax.random.uniform(jax.random.fold_in(own, axis_at), (blocks,), jnp.float32, smallest / len(split), top_value / len(split)))
        gain = gain * jnp.repeat(heights, shape[axis_at] // blocks).reshape([-1 if axis == axis_at else 1 for axis in range(len(shape))])
    return gain


def routed_block(stream_key, own, number, rows, count, top, reach, skew):
    sequence = jax.random.permutation(stream_key, count)
    heavy_load, ordinary = shares(count, rows * top, reach, skew, True), shares(count, rows * top, reach, skew, False)
    places = jnp.arange(count)

    def named(tallies, turn):
        used = int((tallies > 0).sum())
        fixed = max(1, used // 4)
        shifted = fixed + (places - fixed + turn * (used - fixed)) % max(1, count - fixed)
        return jnp.zeros((count,), jnp.int32).at[sequence[jnp.where(places < fixed, places, shifted)]].set(jnp.asarray(tallies, jnp.int32))

    tallies = jnp.where(number % 4 == 0, named(heavy_load, number // 4), named(ordinary, number - number // 4 - 1))
    mixed = jax.random.permutation(jax.random.fold_in(own, 3), count)
    donor, taker = mixed[0:count // 2 * 2:2], mixed[1:count // 2 * 2:2]
    room = jnp.minimum(tallies[donor] - 1, reach - tallies[taker]) // 2
    room = jnp.where((donor == sequence[0]) | (taker == sequence[0]) | (tallies[taker] == 0), 0, jnp.maximum(room, 0))
    shifted = jax.random.randint(jax.random.fold_in(own, 4), (count // 2,), 0, 1 << 20) % (room + 1)
    tallies = tallies.at[donor].add(-shifted).at[taker].add(shifted)
    labels = jnp.searchsorted(jnp.cumsum(tallies), jnp.arange(rows * top), side="right").astype(jnp.int32)
    grid = labels.reshape(top, rows).T
    grid = grid[jax.random.permutation(jax.random.fold_in(own, 1), rows)]
    turn = jax.random.randint(jax.random.fold_in(own, 2), (rows, 1), 0, top)
    return jnp.take_along_axis(grid, (jnp.arange(top)[None, :] + turn) % top, axis=1)


def shares(amount, total, reach, slope, full):
    portions = [(1 << 20) // math.isqrt(grade ** slope) + 1 for grade in range(1, amount + 1)]
    largest = reach if full else min(reach, max(-(-total // amount), total * portions[0] // sum(portions)))
    least = 1 if total - largest >= amount - 1 else 0
    holding, rest = [largest] + [least] * (amount - 1), total - largest - least * (amount - 1)
    while rest > 0:
        candidates = [i for i in range(1, amount) if holding[i] < largest] or [i for i in range(1, amount) if holding[i] < reach]
        mass, budget = sum([portions[i] for i in candidates]), rest
        for i in candidates:
            addition = min(reach - holding[i], max(1, budget * portions[i] // mass), rest)
            holding[i] = holding[i] + addition
            rest = rest - addition
    return np.array(holding)


def noise(own_key, extent, deviation, bound, cuts=(), held_as=jnp.bfloat16):
    result = jax.random.normal(own_key, extent, jnp.float32) * deviation
    if len(cuts) > 0:
        result = level_of(own_key, extent, cuts, -0.22, 0.18) * result
    return jnp.clip(result, min=-bound, max=bound).astype(held_as)


def setup_inputs(seed: int = 0) -> dict:
    arg_keys = jax.random.split(jax.random.key(seed), 19)
    tokens = noise(arg_keys[0], (BATCH, D), 1.0, 6.0, ((0, 16),))
    positions = set_ends(jax.random.randint(arg_keys[1], (BATCH,), 1024, 16384), jax.random.fold_in(arg_keys[1], 1), 1024, 16383).astype(jnp.int32)
    state = noise(arg_keys[2], (BATCH, HEADS, HEAD, HEAD), (2 * HEAD ** -0.5), 1.0, ((0, 16), (1, 2)), jnp.float32)
    mix_gain = jnp.clip(1.0 + 0.18 * jax.random.normal(arg_keys[3], (D,), jnp.float32), 0.1, 1.9)
    w_query = noise(arg_keys[4], (D, HEADS * HEAD), D ** -0.5, 0.125, ((1, 2),))
    w_key = noise(arg_keys[5], (D, HEADS * HEAD), D ** -0.5, 0.125, ((1, 2),))
    w_value = noise(arg_keys[6], (D, HEADS * HEAD), D ** -0.5, 0.125, ((1, 2),))
    w_out = noise(arg_keys[7], (HEADS * HEAD, D), (HEADS * HEAD) ** -0.5, 0.25, ((0, 2),))
    ffn_gain = jnp.clip(1.0 + 0.18 * jax.random.normal(arg_keys[8], (D,), jnp.float32), 0.1, 1.9)
    branch_gate = noise(arg_keys[9], (D,), D ** -0.5, 0.125)
    dense_gate = noise(arg_keys[10], (D, DENSE), D ** -0.5, 0.125, ((0, 2), (1, 16)))
    dense_up = noise(arg_keys[11], (D, DENSE), D ** -0.5, 0.125, ((0, 2), (1, 16)))
    dense_down = noise(arg_keys[12], (DENSE, D), DENSE ** -0.5, 0.09375, ((0, 16), (1, 2)))
    routes_keys = jax.random.split(jax.random.fold_in(arg_keys[13], 1), BATCH // SEQ_DEV)
    routes_turns = jax.random.permutation(jax.random.fold_in(arg_keys[13], 3), BATCH // SEQ_DEV)
    routes = jax.vmap(lambda own, number: routed_block(jax.random.fold_in(arg_keys[13], 2), own, number, SEQ_DEV, EXPERTS, TOP, CAP, 2))(routes_keys, routes_turns).reshape((BATCH, TOP))
    route_scores = jnp.clip(jnp.exp(math.log(1.0) - 2.9957323 * jax.random.uniform(arg_keys[14], (BATCH, TOP), jnp.float32) ** level_of(arg_keys[14], (BATCH, TOP), ((0, 16),), -0.2, 0.2)), 0.05, 1.0)
    expert_gate = noise(arg_keys[15], (EXPERTS, D, EXPERT_W), D ** -0.5, 0.125, ((0, 16), (2, 2)))
    expert_up = noise(arg_keys[16], (EXPERTS, D, EXPERT_W), D ** -0.5, 0.125, ((0, 16), (2, 2)))
    expert_down = noise(arg_keys[17], (EXPERTS, EXPERT_W, D), EXPERT_W ** -0.5, 0.25, ((0, 16), (1, 2)))
    return {"tokens": tokens, "positions": positions, "state": state, "mix_gain": mix_gain, "w_query": w_query, "w_key": w_key, "w_value": w_value, "w_out": w_out, "ffn_gain": ffn_gain, "branch_gate": branch_gate, "dense_gate": dense_gate, "dense_up": dense_up, "dense_down": dense_down, "routes": routes, "route_scores": route_scores, "expert_gate": expert_gate, "expert_up": expert_up, "expert_down": expert_down}


EPS = 1e-06

def normalize(inputs, scale_vec):
    values = inputs.astype(jnp.float32)
    return values * lax.rsqrt(lax.optimization_barrier(jnp.mean(values * values, axis=-1, keepdims=True)) + EPS) * scale_vec

def rotate(vectors, where):
    half = vectors.shape[-1] // 2
    inverse = 1.0 / 10000.0 ** jnp.linspace(0.0, 1.0, half, dtype=jnp.float32)
    angle = where.astype(jnp.float32)[:, None] * inverse[None, :]
    cosine = jnp.cos(angle)[:, None, :]
    sine = jnp.sin(angle)[:, None, :]
    first = vectors[..., :half]
    second = vectors[..., half:]
    return jnp.concatenate([first * cosine - second * sine, second * cosine + first * sine], axis=-1)

def blocked_sum(left, right, blocks):
    inner = left.shape[1] // blocks
    total = jnp.zeros((left.shape[0], right.shape[1]), jnp.float32)
    for block in range(blocks):
        partial_value = jnp.dot(left[:, block * inner:(block + 1) * inner], right[block * inner:(block + 1) * inner], preferred_element_type=jnp.float32)
        rounded = lax.optimization_barrier(partial_value.astype(jnp.bfloat16))
        total = total + rounded.astype(jnp.float32)
    return total

def reference(tokens, positions, state, mix_gain, w_query, w_key, w_value, w_out, ffn_gain, branch_gate, dense_gate, dense_up, dense_down, routes, route_scores, expert_gate, expert_up, expert_down):
    normed = normalize(tokens, mix_gain).astype(jnp.bfloat16)
    query_vec = jnp.dot(normed, w_query, preferred_element_type=jnp.float32).reshape(BATCH, HEADS, HEAD)
    key_vec = jnp.dot(normed, w_key, preferred_element_type=jnp.float32).reshape(BATCH, HEADS, HEAD)
    value_vec = jnp.dot(normed, w_value, preferred_element_type=jnp.float32).reshape(BATCH, HEADS, HEAD)
    query_vec = rotate(query_vec, positions)
    key_vec = rotate(key_vec, positions) * HEAD ** (-0.5)
    head_index = jnp.arange(HEADS, dtype=jnp.float32)
    decay_rate = 1.0 - 2.0 ** (-5.0 - 5.0 * head_index / (HEADS - 1))
    new_state = decay_rate[None, :, None, None] * state + key_vec[:, :, :, None] * value_vec[:, :, None, :]
    retrieved = jnp.einsum('bhd,bhe->bhe', query_vec, jnp.zeros_like(value_vec)) + jnp.einsum('bhd,bhde->bhe', query_vec, new_state, precision=lax.Precision.HIGHEST)
    retrieved = retrieved * lax.rsqrt(lax.optimization_barrier(jnp.mean(retrieved * retrieved, axis=-1, keepdims=True)) + EPS)
    retrieved = retrieved.reshape(BATCH, HEADS * HEAD).astype(jnp.bfloat16)
    mixer_out = blocked_sum(retrieved, w_out, N_TP)
    after_mix = tokens.astype(jnp.float32) + mixer_out
    ffn_in = normalize(after_mix, ffn_gain).astype(jnp.bfloat16)
    per_block = SEQ_DEV * TOP
    chosen = routes.reshape(N_EP, per_block)
    marks = (chosen[:, :, None] == jnp.arange(EXPERTS, dtype=jnp.int32)[None, None, :]).astype(jnp.int32)
    ranking = lax.optimization_barrier(jnp.sum((jnp.cumsum(marks, axis=1) - marks) * marks, axis=2)).astype(jnp.int32)
    source = jnp.broadcast_to(jnp.arange(N_EP, dtype=jnp.int32)[:, None], (N_EP, per_block))
    token_of = (jnp.arange(BATCH * TOP, dtype=jnp.int32) // TOP).reshape(N_EP, per_block)
    buffer = jnp.zeros((EXPERTS, N_EP, CAP, D), jnp.bfloat16).at[chosen, source, ranking].set(ffn_in[token_of])

    def one_expert(pieces):
        rows_in, gate_mat, up_mat, down_mat = pieces
        flat_rows = rows_in.reshape(N_EP * CAP, D)
        gate_pre = jnp.dot(flat_rows, gate_mat, preferred_element_type=jnp.float32)
        up_pre = jnp.dot(flat_rows, up_mat, preferred_element_type=jnp.float32)
        hidden = (jax.nn.silu(gate_pre) * up_pre).astype(jnp.bfloat16)
        return blocked_sum(hidden, down_mat, N_TP).astype(jnp.bfloat16).reshape(N_EP, CAP, D)
    results = lax.map(one_expert, (buffer, expert_gate, expert_up, expert_down))
    picked = results[chosen, source, ranking].reshape(BATCH, TOP, D).astype(jnp.float32)
    route_weights = route_scores / lax.optimization_barrier(jnp.sum(route_scores, axis=1, keepdims=True))
    experts_out = lax.optimization_barrier(jnp.sum(route_weights[:, :, None] * picked, axis=1))
    pre_gate = blocked_sum(ffn_in, dense_gate, N_TP)
    pre_up = blocked_sum(ffn_in, dense_up, N_TP)
    dense_hidden = (jax.nn.silu(pre_gate) * pre_up).astype(jnp.bfloat16)
    dense_out = jnp.dot(dense_hidden, dense_down, preferred_element_type=jnp.float32)
    branch_weight = jax.nn.sigmoid(jnp.dot(ffn_in, branch_gate, preferred_element_type=jnp.float32))
    return (after_mix + experts_out + branch_weight[:, None] * dense_out).astype(jnp.bfloat16)
```

```python
import functools

import jax
import jax.numpy as jnp
from jax import lax
from jax.experimental import pallas as pl
from jax.experimental.pallas import tpu as pltpu
from jax.sharding import PartitionSpec as P

EPS = 1e-06
MESH = pl.DeviceIdType.MESH
F32 = jnp.float32
BF16 = jnp.bfloat16


def normalize(inputs, scale_vec):
    values = inputs.astype(jnp.float32)
    return values * lax.rsqrt(jnp.mean(values * values, axis=-1, keepdims=True) + EPS) * scale_vec


def rotate(vectors, where):
    half = vectors.shape[-1] // 2
    inverse = 1.0 / 10000.0 ** jnp.linspace(0.0, 1.0, half, dtype=jnp.float32)
    angle = where.astype(jnp.float32)[:, None] * inverse[None, :]
    cosine = jnp.cos(angle)[:, None, :]
    sine = jnp.sin(angle)[:, None, :]
    first = vectors[..., :half]
    second = vectors[..., half:]
    return jnp.concatenate(
        [first * cosine - second * sine, second * cosine + first * sine], axis=-1
    )


def split_ep(count):
    inner = 2 if count % 2 == 0 else 1
    rest = count // inner
    middle = 1
    while middle * middle * 4 <= rest and rest % (middle * 2) == 0:
        middle *= 2
    return rest // middle, middle, inner


class Dims:
    pass


def silu(v):
    return v / (1.0 + jnp.exp(-v))


def layer_kernel(n, *refs):
    (tok, hp, side, gain, bgate, eg_h, eu_h, ed_h, dg_h, du_h, dd_h, out,
     eg, eu, ed, dg, du, dd, hpr, am, g, pg, pu, s0, rc, s1, rx, s2, ry, s3, rz,
     w_sem, hp_s, hp_r, ag_s, ag_r, pg_s, pg_r, pu_s, pu_r,
     c_s, c_r, x_s, x_r, y_s, y_r, z_s, z_r) = refs
    A, B, C, T, R, D = n.A, n.B, n.C, n.T, n.R, n.D
    cols, L, NC = n.cols, n.L, n.NC
    cw = cols // NC
    rows = A * B * C * R
    ep = lax.axis_index("ep")
    t = lax.axis_index("tp")
    c = lax.rem(ep, C)
    b = lax.rem(lax.div(ep, C), B)
    a = lax.div(ep, B * C)

    def dev(a_, b_, c_):
        return {"ep": (a_ * B + b_) * C + c_}

    def add(i, d, m):
        return lax.rem(i + d, m)

    def slot(a_, b_, c_):
        return (c_ * B + b_) * A + a_

    def rws(s, count=1):
        return pl.ds(pl.multiple_of(s * R, R), count * R)

    loads = [pltpu.make_async_copy(src, dst, w_sem.at[i]) for i, (src, dst) in enumerate(
        ((dg_h, dg), (du_h, du), (eg_h, eg), (eu_h, eu), (ed_h, ed), (dd_h, dd)))]
    for load in loads:
        load.start()

    bar = pltpu.get_barrier_semaphore()
    peers = [dev(add(a, d, A), b, c) for d in range(1, A)]
    peers += [dev(a, add(b, d, B), c) for d in range(1, B)]
    peers += [dev(a, b, add(c, d, C)) for d in range(1, C)]
    peers += [{"tp": add(t, d, T)} for d in range(1, T)]
    for peer in peers:
        pl.semaphore_signal(bar, inc=1, device_id=peer, device_id_type=MESH)
    pl.semaphore_wait(bar, len(peers))

    sent = []

    def push(src, dst, ss, rs, where):
        copy = pltpu.make_async_remote_copy(
            src_ref=src, dst_ref=dst, send_sem=ss, recv_sem=rs, device_id=where, device_id_type=MESH
        )
        copy.start()
        sent.append(copy)

    def arrived(dst, rs):
        pltpu.make_async_remote_copy(
            src_ref=dst, dst_ref=dst, send_sem=rs, recv_sem=rs, device_id={"tp": t}, device_id_type=MESH
        ).wait_recv()

    for d in range(1, T):
        push(hp, hpr.at[d - 1], hp_s.at[d - 1], hp_r.at[d - 1], {"tp": add(t, d, T)})
    mixed = hp[...].astype(F32)
    for d in range(1, T):
        arrived(hpr.at[d - 1], hp_r.at[d - 1])
        mixed = mixed + hpr[d - 1].astype(F32)
    after = tok[...].astype(F32) + mixed
    am[...] = after
    ffn = (after * lax.rsqrt(jnp.mean(after * after, axis=-1, keepdims=True) + EPS) * gain[...]).astype(BF16)
    score = jnp.sum(ffn.astype(F32) * bgate[...].astype(F32), axis=-1, keepdims=True)
    branch = 1.0 / (1.0 + jnp.exp(-score))
    lane = lax.broadcasted_iota(jnp.int32, (R, L), 1)
    sides = jnp.where(lane == n.E, branch, side[...])
    high = sides.astype(BF16)
    low = (sides - high.astype(F32)).astype(BF16)
    mine = rws(slot(a, b, c))
    g[mine, 0:D] = ffn
    g[mine, D:D + L] = high
    g[mine, D + L:D + 2 * L] = low

    count = 0
    for da in range(1, A):
        push(g.at[mine], g.at[mine], ag_s.at[count], ag_r.at[slot(a, b, c)], dev(add(a, da, A), b, c))
        count += 1
    for da in range(A):
        aa = add(a, da, A)
        own = rws(slot(aa, b, c))
        if da > 0:
            arrived(g.at[own], ag_r.at[slot(aa, b, c)])
        for db in range(1, B):
            push(g.at[own], g.at[own], ag_s.at[count], ag_r.at[slot(aa, b, c)], dev(a, add(b, db, B), c))
            count += 1
        for dc in range(1, C):
            push(g.at[own], g.at[own], ag_s.at[count], ag_r.at[slot(aa, b, c)], dev(a, b, add(c, dc, C)))
            count += 1
    for da in range(A):
        aa = add(a, da, A)
        for db in range(1, B):
            bb = add(b, db, B)
            own = rws(slot(aa, bb, c))
            arrived(g.at[own], ag_r.at[slot(aa, bb, c)])
            for dc in range(1, C):
                push(g.at[own], g.at[own], ag_s.at[count], ag_r.at[slot(aa, bb, c)], dev(a, b, add(c, dc, C)))
                count += 1
    for dc in range(1, C):
        cc = add(c, dc, C)
        for da in range(A):
            for db in range(B):
                ss = slot(add(a, da, A), add(b, db, B), cc)
                arrived(g.at[rws(ss)], ag_r.at[ss])

    loads[0].wait()
    loads[1].wait()
    tile = min(rows, 256)
    own_cols = pl.ds(pl.multiple_of(t * cols, 128), cols)
    for r in range(0, rows, tile):
        xo = g[r:r + tile, own_cols]
        pg[0, r:r + tile, :] = jnp.dot(xo, dg[...], preferred_element_type=F32).astype(BF16)
        pu[0, r:r + tile, :] = jnp.dot(xo, du[...], preferred_element_type=F32).astype(BF16)
    for d in range(1, T):
        push(pg.at[0], pg.at[d], pg_s.at[d - 1], pg_r.at[d - 1], {"tp": add(t, d, T)})
        push(pu.at[0], pu.at[d], pu_s.at[d - 1], pu_r.at[d - 1], {"tp": add(t, d, T)})

    loads[2].wait()
    loads[3].wait()
    K = n.K
    hid, wgt, brw = {}, {}, {}
    for r in range(0, rows, tile):
        lanes = lax.broadcasted_iota(jnp.int32, (tile, L), 1)
        sd = g[r:r + tile, D:D + L].astype(F32) + g[r:r + tile, D + L:D + 2 * L].astype(F32)
        brw[r] = jnp.sum(jnp.where(lanes == n.E, sd, 0.0), axis=1, keepdims=True)
        for k in range(K):
            x = g[r:r + tile, 0:D]
            gate = jnp.dot(x, eg[k], preferred_element_type=F32)
            up = jnp.dot(x, eu[k], preferred_element_type=F32)
            hid[r, k] = (silu(gate) * up).astype(BF16)
            wgt[r, k] = jnp.sum(jnp.where(lanes == ep * K + k, sd, 0.0), axis=1, keepdims=True)
    loads[4].wait()
    loads[5].wait()

    for d in range(1, T):
        arrived(pg.at[d], pg_r.at[d - 1])
        arrived(pu.at[d], pu_r.at[d - 1])
    dense = {}
    for r in range(0, rows, tile):
        pre_g = pg[0, r:r + tile, :].astype(F32)
        pre_u = pu[0, r:r + tile, :].astype(F32)
        for d in range(1, T):
            pre_g = pre_g + pg[d, r:r + tile, :].astype(F32)
            pre_u = pre_u + pu[d, r:r + tile, :].astype(F32)
        dense[r] = (silu(pre_g) * pre_u).astype(BF16)

    per_c, per_b = A * B, A
    def chunk(k):
        return slice(k * cw, (k + 1) * cw)

    def stage0(k):
        for dt in range(T):
            start = pl.multiple_of(add(t, dt, T) * cols + k * cw, 128)
            for r in range(0, rows, tile):
                total = jnp.zeros((tile, cw), F32)
                for e in range(K):
                    total = total + wgt[r, e] * jnp.dot(hid[r, e], ed[e, :, pl.ds(start, cw)], preferred_element_type=F32)
                if dt == 0:
                    total = total + brw[r] * jnp.dot(dense[r], dd[:, chunk(k)], preferred_element_type=F32)
                s0[dt, r:r + tile, chunk(k)] = total.astype(BF16)
            for dc in range(1, C):
                cc = add(c, dc, C)
                i = (k * T + dt) * (C - 1) + dc - 1
                push(s0.at[dt, rws(cc * per_c, per_c), chunk(k)], rc.at[dc - 1, dt, :, chunk(k)],
                     c_s.at[i], c_r.at[i], dev(a, b, cc))

    def stage1(k):
        for dt in list(range(1, T)) + [0]:
            acc = s0[dt, rws(c * per_c, per_c), chunk(k)].astype(F32)
            for dc in range(1, C):
                i = (k * T + dt) * (C - 1) + dc - 1
                arrived(rc.at[dc - 1, dt, :, chunk(k)], c_r.at[i])
                acc = acc + rc[dc - 1, dt, :, chunk(k)].astype(F32)
            s1[dt, :, chunk(k)] = acc.astype(BF16)
            if dt > 0:
                i = k * (T - 1) + dt - 1
                push(s1.at[dt, :, chunk(k)], rx.at[dt - 1, :, chunk(k)], x_s.at[i], x_r.at[i], {"tp": add(t, dt, T)})

    def stage2(k):
        acc = s1[0, :, chunk(k)].astype(F32)
        for dt in range(1, T):
            i = k * (T - 1) + dt - 1
            arrived(rx.at[dt - 1, :, chunk(k)], x_r.at[i])
            acc = acc + rx[dt - 1, :, chunk(k)].astype(F32)
        s2[:, chunk(k)] = acc.astype(BF16)
        for db in range(1, B):
            bb = add(b, db, B)
            i = k * (B - 1) + db - 1
            push(s2.at[rws(bb * per_b, per_b), chunk(k)], ry.at[db - 1, :, chunk(k)], y_s.at[i], y_r.at[i], dev(a, bb, c))

    def stage3(k):
        acc = s2[rws(b * per_b, per_b), chunk(k)].astype(F32)
        for db in range(1, B):
            i = k * (B - 1) + db - 1
            arrived(ry.at[db - 1, :, chunk(k)], y_r.at[i])
            acc = acc + ry[db - 1, :, chunk(k)].astype(F32)
        s3[:, chunk(k)] = acc.astype(BF16)
        for da in range(1, A):
            aa = add(a, da, A)
            i = k * (A - 1) + da - 1
            push(s3.at[rws(aa), chunk(k)], rz.at[da - 1, :, chunk(k)], z_s.at[i], z_r.at[i], dev(aa, b, c))

    def stage4(k):
        acc = s3[rws(a), chunk(k)].astype(F32)
        for da in range(1, A):
            i = k * (A - 1) + da - 1
            arrived(rz.at[da - 1, :, chunk(k)], z_r.at[i])
            acc = acc + rz[da - 1, :, chunk(k)].astype(F32)
        base = am[:, pl.ds(pl.multiple_of(t * cols + k * cw, 128), cw)]
        out[:, chunk(k)] = (base + acc).astype(BF16)

    stages = (stage0, stage1, stage2, stage3, stage4)
    for step in range(NC + len(stages) - 1):
        for s, stage in enumerate(stages):
            if 0 <= step - s < NC:
                stage(step - s)

    for copy in sent:
        copy.wait_send()


def on_device(
    tokens,
    positions,
    state,
    mix_gain,
    w_query,
    w_key,
    w_value,
    w_out,
    ffn_gain,
    branch_gate,
    dense_gate,
    dense_up,
    dense_down,
    routes,
    route_scores,
    expert_gate,
    expert_up,
    expert_down,
):
    sequences = tokens.shape[0]
    model_width = tokens.shape[1]
    tp_count = lax.axis_size("tp")
    ep_count = lax.axis_size("ep")
    columns = model_width // tp_count
    tp_index = lax.axis_index("tp")
    local_heads = state.shape[1]
    head_dim = state.shape[2]
    normed = normalize(tokens, mix_gain).astype(jnp.bfloat16)
    query_vec = jnp.dot(normed, w_query, preferred_element_type=jnp.float32).reshape(
        sequences, local_heads, head_dim
    )
    key_vec = jnp.dot(normed, w_key, preferred_element_type=jnp.float32).reshape(
        sequences, local_heads, head_dim
    )
    value_vec = jnp.dot(normed, w_value, preferred_element_type=jnp.float32).reshape(
        sequences, local_heads, head_dim
    )
    query_vec = rotate(query_vec, positions)
    key_vec = rotate(key_vec, positions) * head_dim ** (-0.5)
    all_heads = local_heads * tp_count
    head_index = (tp_index * local_heads + jnp.arange(local_heads, dtype=jnp.int32)).astype(
        jnp.float32
    )
    decay_rate = 1.0 - 2.0 ** (-5.0 - 5.0 * head_index / (all_heads - 1))
    old = jnp.sum(query_vec[:, :, :, None] * state, axis=2)
    inner = jnp.sum(query_vec * key_vec, axis=2, keepdims=True)
    retrieved = decay_rate[None, :, None] * old + inner * value_vec
    retrieved = retrieved * lax.rsqrt(jnp.mean(retrieved * retrieved, axis=-1, keepdims=True) + EPS)
    retrieved = retrieved.reshape(sequences, local_heads * head_dim).astype(jnp.bfloat16)
    head_partial = jnp.dot(retrieved, w_out, preferred_element_type=jnp.float32).astype(
        jnp.bfloat16
    )

    n = Dims()
    n.A, n.B, n.C = split_ep(ep_count)
    n.T, n.R, n.D, n.cols = tp_count, sequences, model_width, columns
    n.K = expert_gate.shape[0]
    n.E = n.K * ep_count
    n.L = -(-(n.E + 1) // 128) * 128
    n.NC = 2 if columns % 256 == 0 else 1
    route_weights = route_scores / jnp.sum(route_scores, axis=1, keepdims=True)
    marks = routes[:, :, None] == jnp.arange(n.L, dtype=jnp.int32)[None, None, :]
    side = jnp.sum(jnp.where(marks, route_weights[:, :, None], 0.0), axis=1)

    A, B, C, T, R, D, NC = n.A, n.B, n.C, n.T, n.R, n.D, n.NC
    rows = ep_count * R
    hidden = dense_gate.shape[1]
    vm = pl.BlockSpec(memory_space=pltpu.VMEM)
    hbm = pl.BlockSpec(memory_space=pl.ANY)
    dma = pltpu.SemaphoreType.DMA
    vmem = pltpu.VMEM
    part = A * B * R
    scratch = [
        vmem(expert_gate.shape, BF16), vmem(expert_up.shape, BF16), vmem(expert_down.shape, BF16),
        vmem(dense_gate.shape, BF16), vmem(dense_up.shape, BF16), vmem(dense_down.shape, BF16),
        vmem((max(1, T - 1), R, D), BF16), vmem((R, D), F32),
        vmem((rows, D + 2 * n.L), BF16),
        vmem((T, rows, hidden), BF16), vmem((T, rows, hidden), BF16),
        vmem((T, rows, columns), BF16), vmem((max(1, C - 1), T, part, columns), BF16),
        vmem((T, part, columns), BF16), vmem((max(1, T - 1), part, columns), BF16),
        vmem((part, columns), BF16), vmem((max(1, B - 1), A * R, columns), BF16),
        vmem((A * R, columns), BF16), vmem((max(1, A - 1), R, columns), BF16),
        dma((6,)), dma((T,)), dma((T,)), dma((ep_count,)), dma((ep_count,)),
        dma((T,)), dma((T,)), dma((T,)), dma((T,)),
        dma((NC * T * C,)), dma((NC * T * C,)), dma((NC * T,)), dma((NC * T,)),
        dma((NC * B,)), dma((NC * B,)), dma((NC * A,)), dma((NC * A,)),
    ]
    return pl.pallas_call(
        functools.partial(layer_kernel, n),
        out_shape=jax.ShapeDtypeStruct((R, columns), BF16),
        in_specs=[vm] * 5 + [hbm] * 6,
        out_specs=vm,
        scratch_shapes=scratch,
        compiler_params=pltpu.CompilerParams(
            collective_id=0, has_side_effects=True, vmem_limit_bytes=60 * 1024 * 1024
        ),
    )(
        tokens, head_partial, side, ffn_gain[None, :], branch_gate[None, :],
        expert_gate, expert_up, expert_down, dense_gate, dense_up, dense_down,
    )


def solution(mesh):
    placed = (
        P("ep", None),
        P("ep"),
        P("ep", "tp", None, None),
        P(),
        P(None, "tp"),
        P(None, "tp"),
        P(None, "tp"),
        P("tp", None),
        P(),
        P(),
        P("tp", "ep"),
        P("tp", "ep"),
        P("ep", "tp"),
        P("ep", None),
        P("ep", None),
        P("ep", None, "tp"),
        P("ep", None, "tp"),
        P("ep", "tp", None),
    )
    return jax.shard_map(
        on_device, mesh=mesh, in_specs=placed, out_specs=P("ep", "tp"), check_vma=False
    )
```

```python
import functools

import jax
import jax.numpy as jnp
from jax import lax
from jax.experimental import pallas as pl
from jax.experimental.pallas import tpu as pltpu
from jax.sharding import PartitionSpec as P

EPS = 1e-06
MESH = pl.DeviceIdType.MESH
F32 = jnp.float32
BF16 = jnp.bfloat16


def split_ep(count):
    inner = 2 if count % 2 == 0 else 1
    rest = count // inner
    middle = 1
    while middle * middle * 4 <= rest and rest % (middle * 2) == 0:
        middle *= 2
    return rest // middle, middle, inner


class Dims:
    pass


def silu(v):
    return v / (1.0 + jnp.exp(-v))


def layer_kernel(n, *refs):
    (tok, pos, freq, mgain, routes, scores, gain, bgate,
     wq_h, wk_h, wv_h, st_h, wo_h, dg_h, du_h, eg_h, eu_h, ed_h, dd_h, out,
     wq, wk, wv, st, wo, dg, du, eg, eu, ed, dd,
     old, hp, hpr, am, g, pg, pu, s0, rc, s1, rx, s2, ry, s3, rz,
     w_sem, hp_s, hp_r, ag_s, ag_r, pg_s, pg_r, pu_s, pu_r,
     c_s, c_r, x_s, x_r, y_s, y_r, z_s, z_r) = refs
    A, B, C, T, R, D = n.A, n.B, n.C, n.T, n.R, n.D
    cols, S, NC = n.cols, n.S, n.NC
    cw = cols // NC
    ep = lax.axis_index("ep")
    t = lax.axis_index("tp")
    c = lax.rem(ep, C)
    b = lax.rem(lax.div(ep, C), B)
    a = lax.div(ep, B * C)

    def dev(a_, b_, c_):
        return {"ep": (a_ * B + b_) * C + c_}

    def add(i, d, m):
        return lax.rem(i + d, m)

    def slot(a_, b_, c_):
        return (c_ * B + b_) * A + a_

    def rws(s, count=1):
        return pl.ds(pl.multiple_of(s * R, R), count * R)

    names = ("wq", "wk", "wv", "st", "wo", "dg", "du", "eg", "eu", "ed", "dd")
    pairs = ((wq_h, wq), (wk_h, wk), (wv_h, wv), (st_h, st), (wo_h, wo), (dg_h, dg), (du_h, du),
             (eg_h, eg), (eu_h, eu), (ed_h, ed), (dd_h, dd))
    loads = {name: pltpu.make_async_copy(src, dst, w_sem.at[i])
             for i, (name, (src, dst)) in enumerate(zip(names, pairs))}
    for name in names[:5]:
        loads[name].start()

    bar = pltpu.get_barrier_semaphore()
    peers = [dev(add(a, d, A), b, c) for d in range(1, A)]
    peers += [dev(a, add(b, d, B), c) for d in range(1, B)]
    peers += [dev(a, b, add(c, d, C)) for d in range(1, C)]
    peers += [{"tp": add(t, d, T)} for d in range(1, T)]
    for peer in peers:
        pl.semaphore_signal(bar, inc=1, device_id=peer, device_id_type=MESH)

    sent = []

    def push(src, dst, ss, rs, where):
        copy = pltpu.make_async_remote_copy(
            src_ref=src, dst_ref=dst, send_sem=ss, recv_sem=rs, device_id=where, device_id_type=MESH
        )
        copy.start()
        sent.append(copy)

    def arrived(dst, rs):
        pltpu.make_async_remote_copy(
            src_ref=dst, dst_ref=dst, send_sem=rs, recv_sem=rs, device_id={"tp": t}, device_id_type=MESH
        ).wait_recv()

    LH, HD = n.LH, n.HD
    tokens = tok[...].astype(F32)
    normed = (tokens * lax.rsqrt(jnp.mean(tokens * tokens, axis=-1, keepdims=True) + EPS)
              * mgain[...]).astype(BF16)
    angle = pos[...].astype(F32) * freq[...]
    cosine = jnp.cos(angle)
    sine = jnp.sin(angle)
    sine = jnp.where(lax.broadcasted_iota(jnp.int32, (R, HD), 1) < HD // 2, -sine, sine)

    def turn(v):
        return v * cosine + pltpu.roll(v, HD // 2, 1) * sine

    def heads(ref):
        full = jnp.dot(normed, ref[...], preferred_element_type=F32)
        return [full[:, h * HD:(h + 1) * HD] for h in range(LH)]

    loads["wq"].wait()
    query = [turn(v) for v in heads(wq)]
    loads["wk"].wait()
    key = [turn(v) * HD ** (-0.5) for v in heads(wk)]
    loads["wv"].wait()
    value = heads(wv)
    for name in names[5:]:
        loads[name].start()
    loads["st"].wait()
    retrieved = []
    for h in range(LH):
        turned = query[h].T
        for i in range(R):
            old[i:i + 1, h * HD:(h + 1) * HD] = jnp.sum(turned[:, i:i + 1] * st[i, h], axis=0, keepdims=True)
        index = jnp.full((1, HD), t * LH + h, jnp.int32).astype(F32)
        decay = 1.0 - jnp.exp2(-5.0 - 5.0 * index / (LH * T - 1))
        inner = jnp.sum(query[h] * key[h], axis=-1, keepdims=True)
        ret = decay * old[:, h * HD:(h + 1) * HD] + inner * value[h]
        ret = ret * lax.rsqrt(jnp.mean(ret * ret, axis=-1, keepdims=True) + EPS)
        retrieved.append(ret.astype(BF16))
    loads["wo"].wait()
    hp[...] = jnp.dot(jnp.concatenate(retrieved, axis=1), wo[...], preferred_element_type=F32).astype(BF16)
    pl.semaphore_wait(bar, len(peers))

    for d in range(1, T):
        push(hp, hpr.at[d - 1], hp_s.at[d - 1], hp_r.at[d - 1], {"tp": add(t, d, T)})

    lane = lax.broadcasted_iota(jnp.int32, (R, S), 1)
    lane_of = lane % (S // 2)
    marks = scores[...]
    marks = marks / jnp.sum(marks, axis=1, keepdims=True)
    sides = jnp.zeros((R, S), F32)
    for j in range(n.F):
        sides = sides + jnp.where(lane_of == routes[:, j:j + 1], marks[:, j:j + 1], 0.0)

    mixed = hp[...].astype(F32)
    for d in range(1, T):
        arrived(hpr.at[d - 1], hp_r.at[d - 1])
        mixed = mixed + hpr[d - 1].astype(F32)
    after = tokens + mixed
    am[...] = after
    ffn = (after * lax.rsqrt(jnp.mean(after * after, axis=-1, keepdims=True) + EPS) * gain[...]).astype(BF16)
    score = jnp.sum(ffn.astype(F32) * bgate[...].astype(F32), axis=-1, keepdims=True)
    branch = 1.0 / (1.0 + jnp.exp(-score))
    sides = jnp.where(lane_of == n.E, branch, sides)
    high = sides.astype(BF16).astype(F32)
    mine = rws(slot(a, b, c))
    g[mine, 0:D] = ffn
    g[mine, D:D + S] = jnp.where(lane < S // 2, high, sides - high).astype(BF16)

    count = 0
    for da in range(1, A):
        push(g.at[mine], g.at[mine], ag_s.at[count], ag_r.at[slot(a, b, c)], dev(add(a, da, A), b, c))
        count += 1
    for da in range(A):
        aa = add(a, da, A)
        own = rws(slot(aa, b, c))
        if da > 0:
            arrived(g.at[own], ag_r.at[slot(aa, b, c)])
        for db in range(1, B):
            push(g.at[own], g.at[own], ag_s.at[count], ag_r.at[slot(aa, b, c)], dev(a, add(b, db, B), c))
            count += 1
        for dc in range(1, C):
            push(g.at[own], g.at[own], ag_s.at[count], ag_r.at[slot(aa, b, c)], dev(a, b, add(c, dc, C)))
            count += 1

    K = n.K
    GR = A * R
    own_cols = pl.ds(pl.multiple_of(t * cols, 128), cols)
    groups = [(db, dc) for dc in range(C) for db in range(B)]
    hid, wgt, brw, dense = {}, {}, {}, {}

    def group_rows(q):
        return rws(slot(0, add(b, groups[q][0], B), add(c, groups[q][1], C)), A)

    def dense_pre(q):
        gr = group_rows(q)
        x = g[gr, own_cols]
        pg[0, gr, :] = jnp.dot(x, dg[...], preferred_element_type=F32).astype(BF16)
        pu[0, gr, :] = jnp.dot(x, du[...], preferred_element_type=F32).astype(BF16)
        for d in range(1, T):
            i = q * (T - 1) + d - 1
            push(pg.at[0, gr], pg.at[d, gr], pg_s.at[i], pg_r.at[i], {"tp": add(t, d, T)})
            push(pu.at[0, gr], pu.at[d, gr], pu_s.at[i], pu_r.at[i], {"tp": add(t, d, T)})

    def expert_hidden(q):
        gr = group_rows(q)
        sd = g[gr, D:D + S].astype(F32)
        lanes = lax.broadcasted_iota(jnp.int32, (GR, S), 1) % (S // 2)
        brw[q] = jnp.sum(jnp.where(lanes == n.E, sd, 0.0), axis=1, keepdims=True)
        x = g[gr, 0:D]
        for k in range(K):
            gate = jnp.dot(x, eg[k], preferred_element_type=F32)
            up = jnp.dot(x, eu[k], preferred_element_type=F32)
            hid[q, k] = (silu(gate) * up).astype(BF16)
            wgt[q, k] = jnp.sum(jnp.where(lanes == ep * K + k, sd, 0.0), axis=1, keepdims=True)

    def inner_arrived(db, dc):
        for da in range(A):
            ss = slot(add(a, da, A), add(b, db, B), add(c, dc, C))
            arrived(g.at[rws(ss)], ag_r.at[ss])

    for name in ("dg", "du", "eg", "eu"):
        loads[name].wait()
    dense_pre(0)
    expert_hidden(0)
    for db in range(1, B):
        for da in range(A):
            aa, bb = add(a, da, A), add(b, db, B)
            own = rws(slot(aa, bb, c))
            arrived(g.at[own], ag_r.at[slot(aa, bb, c)])
            for dc in range(1, C):
                push(g.at[own], g.at[own], ag_s.at[count], ag_r.at[slot(aa, bb, c)], dev(a, b, add(c, dc, C)))
                count += 1
        dense_pre(db)
    for dc in range(1, C):
        for db in range(B):
            inner_arrived(db, dc)
            dense_pre(dc * B + db)
    for q in range(1, len(groups)):
        expert_hidden(q)
    loads["ed"].wait()
    loads["dd"].wait()

    per_c, per_b = A * B, A

    def chunk(k):
        return slice(k * cw, (k + 1) * cw)

    def stage0(k, dt):
        start = pl.multiple_of(add(t, dt, T) * cols + k * cw, 128)
        order = sorted(range(len(groups)), key=lambda q: -groups[q][1])
        for q in order:
            total = jnp.zeros((GR, cw), F32)
            for e in range(K):
                total = total + wgt[q, e] * jnp.dot(hid[q, e], ed[e, :, pl.ds(start, cw)], preferred_element_type=F32)
            if dt == 0:
                total = total + brw[q] * jnp.dot(dense[q], dd[:, chunk(k)], preferred_element_type=F32)
            s0[dt, group_rows(q), chunk(k)] = total.astype(BF16)
        for dc in range(1, C):
            cc = add(c, dc, C)
            i = (k * T + dt) * (C - 1) + dc - 1
            push(s0.at[dt, rws(cc * per_c, per_c), chunk(k)], rc.at[dc - 1, dt, :, chunk(k)],
                 c_s.at[i], c_r.at[i], dev(a, b, cc))

    def stage1(k, dt):
        acc = s0[dt, rws(c * per_c, per_c), chunk(k)].astype(F32)
        for dc in range(1, C):
            i = (k * T + dt) * (C - 1) + dc - 1
            arrived(rc.at[dc - 1, dt, :, chunk(k)], c_r.at[i])
            acc = acc + rc[dc - 1, dt, :, chunk(k)].astype(F32)
        s1[dt, :, chunk(k)] = acc.astype(BF16)
        if dt > 0:
            i = k * (T - 1) + dt - 1
            push(s1.at[dt, :, chunk(k)], rx.at[dt - 1, :, chunk(k)], x_s.at[i], x_r.at[i], {"tp": add(t, dt, T)})

    def stage2(k):
        acc = s1[0, :, chunk(k)].astype(F32)
        for dt in range(1, T):
            i = k * (T - 1) + dt - 1
            arrived(rx.at[dt - 1, :, chunk(k)], x_r.at[i])
            acc = acc + rx[dt - 1, :, chunk(k)].astype(F32)
        s2[:, chunk(k)] = acc.astype(BF16)
        for db in range(1, B):
            bb = add(b, db, B)
            i = k * (B - 1) + db - 1
            push(s2.at[rws(bb * per_b, per_b), chunk(k)], ry.at[db - 1, :, chunk(k)], y_s.at[i], y_r.at[i], dev(a, bb, c))

    def stage3(k):
        acc = s2[rws(b * per_b, per_b), chunk(k)].astype(F32)
        for db in range(1, B):
            i = k * (B - 1) + db - 1
            arrived(ry.at[db - 1, :, chunk(k)], y_r.at[i])
            acc = acc + ry[db - 1, :, chunk(k)].astype(F32)
        s3[:, chunk(k)] = acc.astype(BF16)
        for da in range(1, A):
            aa = add(a, da, A)
            i = k * (A - 1) + da - 1
            push(s3.at[rws(aa), chunk(k)], rz.at[da - 1, :, chunk(k)], z_s.at[i], z_r.at[i], dev(aa, b, c))

    def stage4(k):
        acc = s3[rws(a), chunk(k)].astype(F32)
        for da in range(1, A):
            i = k * (A - 1) + da - 1
            arrived(rz.at[da - 1, :, chunk(k)], z_r.at[i])
            acc = acc + rz[da - 1, :, chunk(k)].astype(F32)
        base = am[:, pl.ds(pl.multiple_of(t * cols + k * cw, 128), cw)]
        out[:, chunk(k)] = (base + acc).astype(BF16)

    def dense_hidden():
        for q in range(len(groups)):
            gr = group_rows(q)
            for d in range(1, T):
                i = q * (T - 1) + d - 1
                arrived(pg.at[d, gr], pg_r.at[i])
                arrived(pu.at[d, gr], pu_r.at[i])
            pre_g, pre_u = pg[0, gr, :].astype(F32), pu[0, gr, :].astype(F32)
            for d in range(1, T):
                pre_g = pre_g + pg[d, gr, :].astype(F32)
                pre_u = pre_u + pu[d, gr, :].astype(F32)
            dense[q] = (silu(pre_g) * pre_u).astype(BF16)

    far = [(k, dt) for k in range(NC) for dt in range(1, T)]
    for i, item in enumerate(far):
        stage0(*item)
        if i > 0:
            stage1(*far[i - 1])
    dense_hidden()
    if far:
        stage1(*far[-1])
    stages = (lambda k: stage0(k, 0), lambda k: stage1(k, 0), stage2, stage3, stage4)
    for step in range(NC + len(stages) - 1):
        for s, stage in enumerate(stages):
            if 0 <= step - s < NC:
                stage(step - s)

    for copy in sent:
        copy.wait_send()


def on_device(
    tokens,
    positions,
    state,
    mix_gain,
    w_query,
    w_key,
    w_value,
    w_out,
    ffn_gain,
    branch_gate,
    dense_gate,
    dense_up,
    dense_down,
    routes,
    route_scores,
    expert_gate,
    expert_up,
    expert_down,
):
    n = Dims()
    T, ep_count = lax.axis_size("tp"), lax.axis_size("ep")
    A, B, C = split_ep(ep_count)
    R, D = tokens.shape
    columns = D // T
    n.A, n.B, n.C, n.T, n.R, n.D, n.cols = A, B, C, T, R, D, columns
    n.LH, n.HD = state.shape[1], state.shape[2]
    n.F = routes.shape[1]
    n.K = expert_gate.shape[0]
    n.E = n.K * ep_count
    n.S = -(-2 * (n.E + 1) // 128) * 128
    NC = n.NC = columns // 256 if columns % 256 == 0 else 1
    rows = ep_count * R
    hidden = dense_gate.shape[1]
    half = n.HD // 2
    inverse = 1.0 / 10000.0 ** jnp.linspace(0.0, 1.0, half, dtype=jnp.float32)
    freq = jnp.concatenate([inverse, inverse])[None, :]
    vm = pl.BlockSpec(memory_space=pltpu.VMEM)
    hbm = pl.BlockSpec(memory_space=pl.ANY)
    dma = pltpu.SemaphoreType.DMA
    vmem = pltpu.VMEM
    part = A * B * R
    held = [w_query, w_key, w_value, state, w_out, dense_gate, dense_up,
            expert_gate, expert_up, expert_down, dense_down]
    scratch = [vmem(w.shape, w.dtype) for w in held] + [
        vmem((R, n.LH * n.HD), F32), vmem((R, D), BF16),
        vmem((max(1, T - 1), R, D), BF16), vmem((R, D), F32),
        vmem((rows, D + n.S), BF16),
        vmem((T, rows, hidden), BF16), vmem((T, rows, hidden), BF16),
        vmem((T, rows, columns), BF16), vmem((max(1, C - 1), T, part, columns), BF16),
        vmem((T, part, columns), BF16), vmem((max(1, T - 1), part, columns), BF16),
        vmem((part, columns), BF16), vmem((max(1, B - 1), A * R, columns), BF16),
        vmem((A * R, columns), BF16), vmem((max(1, A - 1), R, columns), BF16),
        dma((len(held),)), dma((T,)), dma((T,)), dma((ep_count,)), dma((ep_count,)),
        dma((B * C * T,)), dma((B * C * T,)), dma((B * C * T,)), dma((B * C * T,)),
        dma((NC * T * C,)), dma((NC * T * C,)), dma((NC * T,)), dma((NC * T,)),
        dma((NC * B,)), dma((NC * B,)), dma((NC * A,)), dma((NC * A,)),
    ]
    return pl.pallas_call(
        functools.partial(layer_kernel, n),
        out_shape=jax.ShapeDtypeStruct((R, columns), BF16),
        in_specs=[vm] * 8 + [hbm] * len(held),
        out_specs=vm,
        scratch_shapes=scratch,
        compiler_params=pltpu.CompilerParams(
            collective_id=0, has_side_effects=True, vmem_limit_bytes=60 * 1024 * 1024
        ),
    )(
        tokens, positions[:, None], freq, mix_gain[None, :], routes, route_scores,
        ffn_gain[None, :], branch_gate[None, :], *held,
    )


def solution(mesh):
    placed = (
        P("ep", None),
        P("ep"),
        P("ep", "tp", None, None),
        P(),
        P(None, "tp"),
        P(None, "tp"),
        P(None, "tp"),
        P("tp", None),
        P(),
        P(),
        P("tp", "ep"),
        P("tp", "ep"),
        P("ep", "tp"),
        P("ep", None),
        P("ep", None),
        P("ep", None, "tp"),
        P("ep", None, "tp"),
        P("ep", "tp", None),
    )
    return jax.shard_map(
        on_device, mesh=mesh, in_specs=placed, out_specs=P("ep", "tp"), check_vma=False
    )
```

```python
import functools

import jax
import jax.numpy as jnp
import numpy as np
from jax import lax
from jax.experimental import pallas as pl
from jax.experimental.pallas import tpu as pltpu
from jax.sharding import PartitionSpec as P

EPS = 1e-06
MESH = pl.DeviceIdType.MESH
F32 = jnp.float32
BF16 = jnp.bfloat16


def split_ep(count):
    inner = 2 if count % 2 == 0 else 1
    rest = count // inner
    middle = 1
    while middle * middle * 4 <= rest and rest % (middle * 2) == 0:
        middle *= 2
    return rest // middle, middle, inner


class Dims:
    pass


def silu(v):
    return v / (1.0 + jnp.exp(-v))


def layer_kernel(n, *refs):
    (tok, pos, freq, mgain, routes, scores, gain, bgate,
     wq_h, wk_h, wv_h, st_h, wo_h, dg_h, du_h, eg_h, eu_h, ed_h, dd_h, out,
     wq, wk, wv, st, wo, dg, du, eg, eu, ed, dd,
     old, hp, hpr, am, g, pg, pu, s0, rc, s1, rx, s2, ry, s3, rz,
     w_sem, hp_s, hp_r, ag_s, ag_r, pg_s, pg_r, pu_s, pu_r,
     c_s, c_r, x_s, x_r, y_s, y_r, z_s, z_r) = refs
    A, B, C, T, R, D = n.A, n.B, n.C, n.T, n.R, n.D
    cols, S, NC = n.cols, n.S, n.NC
    cw = cols // NC
    ep = lax.axis_index("ep")
    t = lax.axis_index("tp")
    c = lax.rem(ep, C)
    b = lax.rem(lax.div(ep, C), B)
    a = lax.div(ep, B * C)

    def dev(a_, b_, c_):
        return {"ep": (a_ * B + b_) * C + c_}

    def add(i, d, m):
        return lax.rem(i + d, m)

    def slot(a_, b_, c_):
        return (c_ * B + b_) * A + a_

    def rws(s, count=1):
        return pl.ds(pl.multiple_of(s * R, R), count * R)

    names = ("wq", "wk", "wv", "st", "wo", "dg", "du", "eg", "eu", "ed", "dd")
    pairs = ((wq_h, wq), (wk_h, wk), (wv_h, wv), (st_h, st), (wo_h, wo), (dg_h, dg), (du_h, du),
             (eg_h, eg), (eu_h, eu), (ed_h, ed), (dd_h, dd))
    loads = {name: pltpu.make_async_copy(src, dst, w_sem.at[i])
             for i, (name, (src, dst)) in enumerate(zip(names, pairs))}
    for name in names[:5]:
        loads[name].start()

    bar = pltpu.get_barrier_semaphore()
    peers = [dev(add(a, d, A), b, c) for d in range(1, A)]
    peers += [dev(a, add(b, d, B), c) for d in range(1, B)]
    peers += [dev(a, b, add(c, d, C)) for d in range(1, C)]
    peers += [{"tp": add(t, d, T)} for d in range(1, T)]
    for peer in peers:
        pl.semaphore_signal(bar, inc=1, device_id=peer, device_id_type=MESH)

    sent = []

    def push(src, dst, ss, rs, where):
        copy = pltpu.make_async_remote_copy(
            src_ref=src, dst_ref=dst, send_sem=ss, recv_sem=rs, device_id=where, device_id_type=MESH
        )
        copy.start()
        sent.append(copy)

    def arrived(dst, rs):
        pltpu.make_async_remote_copy(
            src_ref=dst, dst_ref=dst, send_sem=rs, recv_sem=rs, device_id={"tp": t}, device_id_type=MESH
        ).wait_recv()

    LH, HD = n.LH, n.HD
    tokens = tok[...].astype(F32)
    normed = (tokens * lax.rsqrt(jnp.mean(tokens * tokens, axis=-1, keepdims=True) + EPS)
              * mgain[...]).astype(BF16)
    eye = lax.broadcasted_iota(jnp.int32, (R, R), 0) == lax.broadcasted_iota(jnp.int32, (R, R), 1)

    def column(row):
        return jnp.sum(jnp.where(eye, row.astype(F32), 0.0), axis=1, keepdims=True)

    angle = column(pos[...]) * freq[...]
    cosine = jnp.cos(angle)
    sine = jnp.sin(angle)
    sine = jnp.where(lax.broadcasted_iota(jnp.int32, (R, HD), 1) < HD // 2, -sine, sine)

    def turn(v):
        return v * cosine + pltpu.roll(v, HD // 2, 1) * sine

    def heads(ref):
        full = jnp.dot(normed, ref[...], preferred_element_type=F32)
        return [full[:, h * HD:(h + 1) * HD] for h in range(LH)]

    loads["wq"].wait()
    query = [turn(v) for v in heads(wq)]
    loads["wk"].wait()
    key = [turn(v) * HD ** (-0.5) for v in heads(wk)]
    loads["wv"].wait()
    value = heads(wv)
    for name in names[5:]:
        loads[name].start()
    loads["st"].wait()
    retrieved = []
    for h in range(LH):
        turned = query[h].T
        for i in range(R):
            old[i:i + 1, h * HD:(h + 1) * HD] = jnp.sum(turned[:, i:i + 1] * st[i, h], axis=0, keepdims=True)
        index = jnp.full((1, HD), t * LH + h, jnp.int32).astype(F32)
        decay = 1.0 - jnp.exp2(-5.0 - 5.0 * index / (LH * T - 1))
        inner = jnp.sum(query[h] * key[h], axis=-1, keepdims=True)
        ret = decay * old[:, h * HD:(h + 1) * HD] + inner * value[h]
        ret = ret * lax.rsqrt(jnp.mean(ret * ret, axis=-1, keepdims=True) + EPS)
        retrieved.append(ret.astype(BF16))
    loads["wo"].wait()
    hp[...] = jnp.dot(jnp.concatenate(retrieved, axis=1), wo[...], preferred_element_type=F32).astype(BF16)
    pl.semaphore_wait(bar, len(peers))

    for d in range(1, T):
        push(hp, hpr.at[d - 1], hp_s.at[d - 1], hp_r.at[d - 1], {"tp": add(t, d, T)})

    lane = lax.broadcasted_iota(jnp.int32, (R, S), 1)
    lane_of = lane % (S // 2)
    shares = scores[...]
    shares = shares / jnp.sum(shares, axis=0, keepdims=True)
    chosen = routes[...]
    sides = jnp.zeros((R, S), F32)
    for j in range(n.F):
        sides = sides + jnp.where(lane_of.astype(F32) == column(chosen[j:j + 1]), column(shares[j:j + 1]), 0.0)

    mixed = hp[...].astype(F32)
    for d in range(1, T):
        arrived(hpr.at[d - 1], hp_r.at[d - 1])
        mixed = mixed + hpr[d - 1].astype(F32)
    after = tokens + mixed
    am[...] = after
    ffn = (after * lax.rsqrt(jnp.mean(after * after, axis=-1, keepdims=True) + EPS) * gain[...]).astype(BF16)
    score = jnp.zeros((R, 128), F32)
    for j in range(D // 128):
        score = score + ffn[:, j * 128:(j + 1) * 128].astype(F32) * bgate[j:j + 1, :].astype(F32)
    score = jnp.sum(score, axis=-1, keepdims=True)
    branch = 1.0 / (1.0 + jnp.exp(-score))
    sides = jnp.where(lane_of == n.E, branch, sides)
    high = sides.astype(BF16).astype(F32)
    mine = rws(slot(a, b, c))
    g[mine, 0:D] = ffn
    g[mine, D:D + S] = jnp.where(lane < S // 2, high, sides - high).astype(BF16)

    count = 0
    for da in range(1, A):
        push(g.at[mine], g.at[mine], ag_s.at[count], ag_r.at[slot(a, b, c)], dev(add(a, da, A), b, c))
        count += 1
    for da in range(A):
        aa = add(a, da, A)
        own = rws(slot(aa, b, c))
        if da > 0:
            arrived(g.at[own], ag_r.at[slot(aa, b, c)])
        for db in range(1, B):
            push(g.at[own], g.at[own], ag_s.at[count], ag_r.at[slot(aa, b, c)], dev(a, add(b, db, B), c))
            count += 1
        for dc in range(1, C):
            push(g.at[own], g.at[own], ag_s.at[count], ag_r.at[slot(aa, b, c)], dev(a, b, add(c, dc, C)))
            count += 1

    K = n.K
    GR = A * R
    own_cols = pl.ds(pl.multiple_of(t * cols, 128), cols)
    groups = [(db, dc) for dc in range(C) for db in range(B)]
    hid, wgt, brw, dense = {}, {}, {}, {}

    def group_rows(q):
        return rws(slot(0, add(b, groups[q][0], B), add(c, groups[q][1], C)), A)

    def dense_pre(q):
        gr = group_rows(q)
        x = g[gr, own_cols]
        pg[0, gr, :] = jnp.dot(x, dg[...], preferred_element_type=F32).astype(BF16)
        pu[0, gr, :] = jnp.dot(x, du[...], preferred_element_type=F32).astype(BF16)
        for d in range(1, T):
            i = q * (T - 1) + d - 1
            push(pg.at[0, gr], pg.at[d, gr], pg_s.at[i], pg_r.at[i], {"tp": add(t, d, T)})
            push(pu.at[0, gr], pu.at[d, gr], pu_s.at[i], pu_r.at[i], {"tp": add(t, d, T)})

    def expert_hidden(q):
        gr = group_rows(q)
        sd = g[gr, D:D + S].astype(F32)
        lanes = lax.broadcasted_iota(jnp.int32, (GR, S), 1) % (S // 2)
        brw[q] = jnp.sum(jnp.where(lanes == n.E, sd, 0.0), axis=1, keepdims=True)
        x = g[gr, 0:D]
        for k in range(K):
            gate = jnp.dot(x, eg[k], preferred_element_type=F32)
            up = jnp.dot(x, eu[k], preferred_element_type=F32)
            hid[q, k] = (silu(gate) * up).astype(BF16)
            wgt[q, k] = jnp.sum(jnp.where(lanes == ep * K + k, sd, 0.0), axis=1, keepdims=True)

    def inner_arrived(db, dc):
        for da in range(A):
            ss = slot(add(a, da, A), add(b, db, B), add(c, dc, C))
            arrived(g.at[rws(ss)], ag_r.at[ss])

    for name in ("dg", "du", "eg", "eu"):
        loads[name].wait()
    dense_pre(0)
    expert_hidden(0)
    for db in range(1, B):
        for da in range(A):
            aa, bb = add(a, da, A), add(b, db, B)
            own = rws(slot(aa, bb, c))
            arrived(g.at[own], ag_r.at[slot(aa, bb, c)])
            for dc in range(1, C):
                push(g.at[own], g.at[own], ag_s.at[count], ag_r.at[slot(aa, bb, c)], dev(a, b, add(c, dc, C)))
                count += 1
        dense_pre(db)
        expert_hidden(db)
    for dc in range(1, C):
        for db in range(B):
            inner_arrived(db, dc)
            dense_pre(dc * B + db)
    for q in range(B, len(groups)):
        expert_hidden(q)
    loads["ed"].wait()
    loads["dd"].wait()

    per_c, per_b = A * B, A

    def chunk(k):
        return slice(k * cw, (k + 1) * cw)

    def stage0(k, dt):
        start = pl.multiple_of(add(t, dt, T) * cols + k * cw, 128)
        order = sorted(range(len(groups)), key=lambda q: -groups[q][1])
        for q in order:
            total = jnp.zeros((GR, cw), F32)
            for e in range(K):
                total = total + wgt[q, e] * jnp.dot(hid[q, e], ed[e, :, pl.ds(start, cw)], preferred_element_type=F32)
            if dt == 0:
                total = total + brw[q] * jnp.dot(dense[q], dd[:, chunk(k)], preferred_element_type=F32)
            s0[k, dt, group_rows(q)] = total.astype(BF16)
        for dc in range(1, C):
            cc = add(c, dc, C)
            i = (k * T + dt) * (C - 1) + dc - 1
            push(s0.at[k, dt, rws(cc * per_c, per_c)], rc.at[k, dc - 1, dt],
                 c_s.at[i], c_r.at[i], dev(a, b, cc))

    def stage1(k, dt):
        acc = s0[k, dt, rws(c * per_c, per_c)].astype(F32)
        for dc in range(1, C):
            i = (k * T + dt) * (C - 1) + dc - 1
            arrived(rc.at[k, dc - 1, dt], c_r.at[i])
            acc = acc + rc[k, dc - 1, dt].astype(F32)
        s1[k, dt] = acc.astype(BF16)
        if dt > 0:
            i = k * (T - 1) + dt - 1
            push(s1.at[k, dt], rx.at[k, dt - 1], x_s.at[i], x_r.at[i], {"tp": add(t, dt, T)})

    def stage2(k):
        acc = s1[k, 0].astype(F32)
        for dt in range(1, T):
            i = k * (T - 1) + dt - 1
            arrived(rx.at[k, dt - 1], x_r.at[i])
            acc = acc + rx[k, dt - 1].astype(F32)
        s2[k] = acc.astype(BF16)
        for db in range(1, B):
            bb = add(b, db, B)
            i = k * (B - 1) + db - 1
            push(s2.at[k, rws(bb * per_b, per_b)], ry.at[k, db - 1], y_s.at[i], y_r.at[i], dev(a, bb, c))

    def stage3(k):
        acc = s2[k, rws(b * per_b, per_b)].astype(F32)
        for db in range(1, B):
            i = k * (B - 1) + db - 1
            arrived(ry.at[k, db - 1], y_r.at[i])
            acc = acc + ry[k, db - 1].astype(F32)
        s3[k] = acc.astype(BF16)
        for da in range(1, A):
            aa = add(a, da, A)
            i = k * (A - 1) + da - 1
            push(s3.at[k, rws(aa)], rz.at[k, da - 1], z_s.at[i], z_r.at[i], dev(aa, b, c))

    def stage4(k):
        acc = s3[k, rws(a)].astype(F32)
        for da in range(1, A):
            i = k * (A - 1) + da - 1
            arrived(rz.at[k, da - 1], z_r.at[i])
            acc = acc + rz[k, da - 1].astype(F32)
        base = am[:, pl.ds(pl.multiple_of(t * cols + k * cw, 128), cw)]
        out[:, chunk(k)] = (base + acc).astype(BF16)

    def dense_hidden():
        for q in range(len(groups)):
            gr = group_rows(q)
            for d in range(1, T):
                i = q * (T - 1) + d - 1
                arrived(pg.at[d, gr], pg_r.at[i])
                arrived(pu.at[d, gr], pu_r.at[i])
            pre_g, pre_u = pg[0, gr, :].astype(F32), pu[0, gr, :].astype(F32)
            for d in range(1, T):
                pre_g = pre_g + pg[d, gr, :].astype(F32)
                pre_u = pre_u + pu[d, gr, :].astype(F32)
            dense[q] = (silu(pre_g) * pre_u).astype(BF16)

    far = [(k, dt) for k in range(NC) for dt in range(1, T)]
    for i, item in enumerate(far):
        stage0(*item)
        if i > 0:
            stage1(*far[i - 1])
    dense_hidden()
    if far:
        stage1(*far[-1])
    stages = (lambda k: stage0(k, 0), lambda k: stage1(k, 0), stage2, stage3, stage4)
    for step in range(NC + len(stages) - 1):
        for s, stage in enumerate(stages):
            if 0 <= step - s < NC:
                stage(step - s)

    for copy in sent:
        copy.wait_send()


def on_device(
    tokens,
    positions,
    state,
    mix_gain,
    w_query,
    w_key,
    w_value,
    w_out,
    ffn_gain,
    branch_gate,
    dense_gate,
    dense_up,
    dense_down,
    routes,
    route_scores,
    expert_gate,
    expert_up,
    expert_down,
):
    n = Dims()
    T, ep_count = lax.axis_size("tp"), lax.axis_size("ep")
    A, B, C = split_ep(ep_count)
    R, D = tokens.shape
    columns = D // T
    n.A, n.B, n.C, n.T, n.R, n.D, n.cols = A, B, C, T, R, D, columns
    n.LH, n.HD = state.shape[1], state.shape[2]
    n.F = routes.shape[1]
    n.K = expert_gate.shape[0]
    n.E = n.K * ep_count
    n.S = -(-2 * (n.E + 1) // 128) * 128
    NC = n.NC = columns // 512 if columns % 512 == 0 else 1
    wide = columns // NC
    rows = ep_count * R
    hidden = dense_gate.shape[1]
    half = n.HD // 2
    inverse = 1.0 / 10000.0 ** (np.arange(half) / (half - 1))
    freq = np.concatenate([inverse, inverse])[None, :].astype(np.float32)
    vm = pl.BlockSpec(memory_space=pltpu.VMEM)
    hbm = pl.BlockSpec(memory_space=pl.ANY)
    dma = pltpu.SemaphoreType.DMA
    vmem = pltpu.VMEM
    part = A * B * R
    held = [w_query, w_key, w_value, state, w_out, dense_gate, dense_up,
            expert_gate, expert_up, expert_down, dense_down]
    scratch = [vmem(w.shape, w.dtype) for w in held] + [
        vmem((R, n.LH * n.HD), F32), vmem((R, D), BF16),
        vmem((max(1, T - 1), R, D), BF16), vmem((R, D), F32),
        vmem((rows, D + n.S), BF16),
        vmem((T, rows, hidden), BF16), vmem((T, rows, hidden), BF16),
        vmem((NC, T, rows, wide), BF16), vmem((NC, max(1, C - 1), T, part, wide), BF16),
        vmem((NC, T, part, wide), BF16), vmem((NC, max(1, T - 1), part, wide), BF16),
        vmem((NC, part, wide), BF16), vmem((NC, max(1, B - 1), A * R, wide), BF16),
        vmem((NC, A * R, wide), BF16), vmem((NC, max(1, A - 1), R, wide), BF16),
        dma((len(held),)), dma((T,)), dma((T,)), dma((ep_count,)), dma((ep_count,)),
        dma((B * C * T,)), dma((B * C * T,)), dma((B * C * T,)), dma((B * C * T,)),
        dma((NC * T * C,)), dma((NC * T * C,)), dma((NC * T,)), dma((NC * T,)),
        dma((NC * B,)), dma((NC * B,)), dma((NC * A,)), dma((NC * A,)),
    ]
    return pl.pallas_call(
        functools.partial(layer_kernel, n),
        out_shape=jax.ShapeDtypeStruct((R, columns), BF16),
        in_specs=[vm] * 8 + [hbm] * len(held),
        out_specs=vm,
        scratch_shapes=scratch,
        compiler_params=pltpu.CompilerParams(
            collective_id=0, has_side_effects=True, vmem_limit_bytes=60 * 1024 * 1024
        ),
    )(
        tokens, positions[None, :], freq, mix_gain[None, :], routes.T, route_scores.T,
        ffn_gain[None, :], branch_gate.reshape(D // 128, 128), *held,
    )


def solution(mesh):
    placed = (
        P("ep", None),
        P("ep"),
        P("ep", "tp", None, None),
        P(),
        P(None, "tp"),
        P(None, "tp"),
        P(None, "tp"),
        P("tp", None),
        P(),
        P(),
        P("tp", "ep"),
        P("tp", "ep"),
        P("ep", "tp"),
        P("ep", None),
        P("ep", None),
        P("ep", None, "tp"),
        P("ep", None, "tp"),
        P("ep", "tp", None),
    )
    return jax.shard_map(
        on_device, mesh=mesh, in_specs=placed, out_specs=P("ep", "tp"), check_vma=False
    )
```
